32 devices in a mesh: sp: 8 (over z, y), tp: 4 (over x, core).
Axes of the slice: x: 2, y: 2, z: 4, core: 2. Of those that a mesh axis runs over, the one named last changes fastest.
Arguments:
- inputs: bfloat16 [12288, 2048], P('sp'), may hold values from -6 to 6
- norm_gain: float32 [2048], replicated, may hold values from 0.1 to 1.9
- pool_weight: bfloat16 [2048, 1024], P(None, 'tp'), may hold values from -0.125 to 0.125
- query_weight: bfloat16 [2048, 1024], P(None, 'tp'), may hold values from -0.125 to 0.125
- forget_weight: bfloat16 [2048, 1024], P(None, 'tp'), may hold values from -0.125 to 0.125
- value_weight: bfloat16 [2048, 1024], P(None, 'tp'), may hold values from -0.125 to 0.125
- outgate_weight: bfloat16 [2048, 1024], P(None, 'tp'), may hold values from -0.125 to 0.125
- pool_mix: bfloat16 [4, 256, 256], P('tp'), may hold values from -0.375 to 0.375
- pool_scale: float32 [1024], P('tp'), may hold values from 0.1 to 1.9
- lower_bound: float32 [1024], P('tp'), may hold values from 0.9 to 1
- extra_decay: float32 [12288, 8], P('sp', 'tp'), may hold values from -1 to 0
- recur_gain: float32 [1024], P('tp'), may hold values from 0.1 to 1.9
- init_state: float32 [8, 128, 128], P('tp'), may hold values from -0.013531647 to 0.013531647
- out_pool: bfloat16 [1024, 2048], P('tp'), may hold values from -0.125 to 0.125
- out_recur: bfloat16 [1024, 2048], P('tp'), may hold values from -0.125 to 0.125
Outputs:
- mixed: bfloat16 [12288, 2048], P(('sp', 'tp'))
The draws below stay inside these ranges and needn't reach their ends.
All inputs are finite; a program needn't handle non-finite values.
Results may differ from the reference program's by a relative error of at most 0.014.
Values may be sent and summed in bfloat16 or wider, within the bound.
A program may use at most 128 MiB of HBM per device.

```python
import jax
import jax.numpy as jnp
from jax import lax

D = 2048
BRANCH = 1024
GROUPS = 4
HEAD_K = 128
BLOCK = 64
TOK_DEV = 1536
GROUP_W = 256
HEADS = 8
SEQUENCE_LENGTH = 12288


def draw_lower_bound(key, part):
    count_of_heads = BRANCH // HEAD_K
    key_slow, key_fast, key_pick = jax.random.split(jax.random.fold_in(key, 11), 3)
    slow_gap = jnp.exp(jax.random.uniform(key_slow, (BRANCH,), jnp.float32, jnp.log(0.15), 0.0)) / SEQUENCE_LENGTH
    fast_head = jax.random.bernoulli(key_pick, 0.5, (count_of_heads,))
    fast_gap = jnp.exp(jax.random.uniform(key_fast, (BRANCH,), jnp.float32, jnp.log(0.03), jnp.log(0.08)))
    fast_channel = jnp.repeat(fast_head, HEAD_K)
    gap = jnp.where(fast_channel, fast_gap, slow_gap)
    return (1.0 - gap).astype(jnp.float32)


def draw_extra_decay(key, part):
    count_of_heads = BRANCH // HEAD_K
    key_rate, key_location, key_depth = jax.random.split(jax.random.fold_in(key, 23), 3)
    span_count = SEQUENCE_LENGTH // TOK_DEV
    rate = jnp.exp(jax.random.uniform(key_rate, (span_count, count_of_heads), jnp.float32, jnp.log(0.1), jnp.log(0.6)))
    base_offset = -jnp.repeat(rate, TOK_DEV, axis=0) / SEQUENCE_LENGTH
    spurt_rows = jax.random.randint(key_location, (2, count_of_heads), 0, SEQUENCE_LENGTH)
    layer_depth = jnp.log(jax.random.uniform(key_depth, (2, count_of_heads), jnp.float32, 0.55, 0.8))
    token_positions = jnp.arange(SEQUENCE_LENGTH, dtype=jnp.int32)[:, None, None]
    spurt_list = jnp.sum(jnp.where(token_positions == spurt_rows[None], layer_depth[None], 0.0), axis=1)
    return (base_offset + spurt_list).astype(jnp.float32)


def steps_of(rng, extent, cuts, low, high):
    level, own = 1.0, jax.random.fold_in(rng, 6)
    for position, shards_of in cuts:
        draws = jnp.exp(jax.random.uniform(jax.random.fold_in(own, position), (shards_of,), jnp.float32, low / len(cuts), high / len(cuts)))
        level = level * jnp.repeat(draws, extent[position] // shards_of).reshape([-1 if axis == position else 1 for axis in range(len(extent))])
    return level


def noise(own_key, shape, deviation, limit, cuts=(), kind=jnp.bfloat16):
    drawn = jax.random.normal(own_key, shape, jnp.float32) * deviation
    if len(cuts) > 0:
        drawn = steps_of(own_key, shape, cuts, -0.22, 0.18) * drawn
    return jnp.clip(drawn, min=-limit, max=limit).astype(kind)


def setup_inputs(seed: int = 0) -> dict:
    splits = jax.random.split(jax.random.key(seed), 16)
    inputs = noise(splits[0], (SEQUENCE_LENGTH, D), 1.0, 6.0, ((0, 8),))
    norm_gain = jnp.clip(1.0 + 0.18 * jax.random.normal(splits[1], (D,), jnp.float32), 0.1, 1.9)
    pool_weight = noise(splits[2], (D, BRANCH), D ** -0.5, 0.125, ((1, 4),))
    query_weight = noise(splits[3], (D, BRANCH), D ** -0.5, 0.125, ((1, 4),))
    forget_weight = noise(splits[4], (D, BRANCH), D ** -0.5, 0.125, ((1, 4),))
    value_weight = noise(splits[5], (D, BRANCH), D ** -0.5, 0.125, ((1, 4),))
    outgate_weight = noise(splits[6], (D, BRANCH), D ** -0.5, 0.125, ((1, 4),))
    pool_mix = noise(splits[7], (GROUPS, GROUP_W, GROUP_W), GROUP_W ** -0.5, 0.375, ((0, 4),))
    pool_scale = jnp.clip(1.0 + 0.18 * jax.random.normal(splits[8], (BRANCH,), jnp.float32), 0.1, 1.9)
    lower_bound = draw_lower_bound(jax.random.fold_in(splits[15], 71), 0)
    extra_decay = draw_extra_decay(jax.random.fold_in(splits[15], 71), 0)
    recur_gain = jnp.clip(1.0 + 0.18 * jax.random.normal(splits[11], (BRANCH,), jnp.float32), 0.1, 1.9)
    init_state = noise(splits[12], (HEADS, HEAD_K, HEAD_K), (0.25 * SEQUENCE_LENGTH ** -0.5), 0.013531647, ((0, 4),), jnp.float32)
    out_pool = noise(splits[13], (BRANCH, D), (2 * BRANCH) ** -0.5, 0.125, ((0, 4),))
    out_recur = noise(splits[14], (BRANCH, D), (2 * BRANCH) ** -0.5, 0.125, ((0, 4),))
    return dict(inputs=inputs, norm_gain=norm_gain, pool_weight=pool_weight, query_weight=query_weight, forget_weight=forget_weight, value_weight=value_weight, outgate_weight=outgate_weight, pool_mix=pool_mix, pool_scale=pool_scale, lower_bound=lower_bound, extra_decay=extra_decay, recur_gain=recur_gain, init_state=init_state, out_pool=out_pool, out_recur=out_recur)


norm_eps = 1e-05
top_precision = lax.Precision.HIGHEST

def norm_rows(array, scale_vec):
    widened = array.astype(jnp.float32)
    scaled = widened * lax.rsqrt(lax.optimization_barrier(jnp.mean(widened * widened, axis=-1, keepdims=True)) + norm_eps)
    return (scaled * scale_vec).astype(jnp.bfloat16)

def window_sums(widened):
    results = []
    current = widened
    for level_idx in range(GROUPS):
        stride = 2 ** level_idx
        shifted = jnp.pad(current, ((stride, 0), (0, 0)))[:current.shape[0]]
        current = current + shifted
        results.append(current)
    return results

def pool_branch(pool_in, pool_mix, pool_scale):
    row_count = pool_in.shape[0]
    group_width = pool_mix.shape[1]
    widened = pool_in.astype(jnp.float32)
    window_totals = window_sums(widened)
    token_positions = jnp.arange(row_count, dtype=jnp.int32)
    pieces = []
    for group_idx in range(pool_mix.shape[0]):
        columns = slice(group_idx * group_width, (group_idx + 1) * group_width)
        reach = jnp.minimum(token_positions + 1, 2 ** (group_idx + 1)).astype(jnp.float32)
        pieces.append(window_totals[group_idx][:, columns] / reach[:, None] - widened[:, columns])
    pooled = jnp.stack(pieces, axis=1).astype(jnp.bfloat16)
    mixed_groups = jnp.einsum('rgc,gcd->rgd', pooled.astype(jnp.float32), pool_mix.astype(jnp.float32))
    return (mixed_groups.reshape(row_count, -1) * pool_scale).astype(jnp.bfloat16)

def recur_inputs(query_raw, forget_raw, value_raw, bound_vec, extra_log, head_k, block_len):
    row_count = query_raw.shape[0]
    count_of_heads = query_raw.shape[1] // head_k
    block_count = row_count // block_len
    forget_pre = forget_raw.astype(jnp.float32)
    log_f = jnp.logaddexp(jnp.log(bound_vec), jnp.log1p(-bound_vec) + jax.nn.log_sigmoid(forget_pre))
    log_f = log_f.reshape(row_count, count_of_heads, head_k) + extra_log[:, :, None]
    key_input = ((1.0 - bound_vec) * jax.nn.sigmoid(-forget_pre)).reshape(row_count, count_of_heads, head_k)
    query_input = jax.nn.silu(query_raw.astype(jnp.float32)).reshape(row_count, count_of_heads, head_k)
    value_input = value_raw.astype(jnp.float32).reshape(row_count, count_of_heads, head_k)

    def to_blocks(array):
        return array.reshape(block_count, block_len, count_of_heads, head_k).transpose(2, 0, 1, 3)
    return (to_blocks(query_input), to_blocks(key_input), to_blocks(value_input), to_blocks(log_f))

def block_parts(query_input, key_input, value_input, log_f):
    block_len = log_f.shape[2]
    cum_log = jnp.cumsum(log_f, axis=2)
    last_log = cum_log[:, :, -1:, :]
    query_dec = query_input * jnp.exp(cum_log)
    key_dec = key_input * jnp.exp(-cum_log)
    scores = jnp.einsum('hntk,hnsk->hnts', query_dec, key_dec, precision=top_precision)
    causal = jnp.tril(jnp.ones((block_len, block_len), dtype=bool))
    scores = jnp.where(causal, scores, 0.0)
    within = jnp.einsum('hnts,hnsv->hntv', scores, value_input, precision=top_precision)
    contrib = jnp.einsum('hnsk,hnsv->hnkv', key_input * jnp.exp(last_log - cum_log), value_input, precision=top_precision)
    decays = jnp.exp(last_log[:, :, 0, :])
    return (query_dec, within, decays, contrib)

def chain(earlier, later_part):
    return (earlier[0] * later_part[0], later_part[0][..., None] * earlier[1] + later_part[1])

def recur_branch(query_raw, forget_raw, value_raw, outgate_raw, bound_vec, extra_log, recur_gain, init_state):
    row_count = query_raw.shape[0]
    head_k = init_state.shape[1]
    count_of_heads = init_state.shape[0]
    query_in, key_in, value_in, log_f = recur_inputs(query_raw, forget_raw, value_raw, bound_vec, extra_log, head_k, BLOCK)
    query_dec, within, decays, contrib = block_parts(query_in, key_in, value_in, log_f)
    running = lax.associative_scan(chain, (decays, contrib), axis=1)
    enter_a = jnp.concatenate([jnp.ones_like(decays[:, :1]), running[0][:, :-1]], axis=1)
    enter_s = jnp.concatenate([jnp.zeros_like(contrib[:, :1]), running[1][:, :-1]], axis=1)
    state_in = enter_s + enter_a[..., None] * init_state[:, None]
    recur_out = within + jnp.einsum('hntk,hnkv->hntv', query_dec, state_in, precision=top_precision)
    recur_out = recur_out.transpose(1, 2, 0, 3).reshape(row_count, count_of_heads, head_k)
    recur_out = recur_out * lax.rsqrt(lax.optimization_barrier(jnp.mean(recur_out * recur_out, axis=-1, keepdims=True)) + norm_eps)
    recur_out = recur_out * recur_gain.reshape(count_of_heads, head_k)
    gated = recur_out.reshape(row_count, count_of_heads * head_k) * jax.nn.silu(outgate_raw.astype(jnp.float32))
    return gated.astype(jnp.bfloat16)

def reference(inputs, norm_gain, pool_weight, query_weight, forget_weight, value_weight, outgate_weight, pool_mix, pool_scale, lower_bound, extra_decay, recur_gain, init_state, out_pool, out_recur):
    normed = norm_rows(inputs, norm_gain)
    pool_in = jnp.dot(normed, pool_weight, preferred_element_type=jnp.float32).astype(jnp.bfloat16)
    query_raw = jnp.dot(normed, query_weight, preferred_element_type=jnp.float32).astype(jnp.bfloat16)
    forget_raw = jnp.dot(normed, forget_weight, preferred_element_type=jnp.float32).astype(jnp.bfloat16)
    value_raw = jnp.dot(normed, value_weight, preferred_element_type=jnp.float32).astype(jnp.bfloat16)
    outgate_raw = jnp.dot(normed, outgate_weight, preferred_element_type=jnp.float32).astype(jnp.bfloat16)
    y_pool = pool_branch(pool_in, pool_mix, pool_scale)
    y_recur = recur_branch(query_raw, forget_raw, value_raw, outgate_raw, lower_bound, extra_decay, recur_gain, init_state)
    summed = jnp.dot(y_pool, out_pool, preferred_element_type=jnp.float32)
    summed = summed + jnp.dot(y_recur, out_recur, preferred_element_type=jnp.float32)
    return summed.astype(jnp.bfloat16)
```

```python
import functools
import jax
import jax.numpy as jnp
from jax import lax
from jax.experimental import pallas as pl
from jax.experimental.pallas import tpu as pltpu
from jax.sharding import PartitionSpec as P

NORM_EPS = 1e-05
HALO = 16
CHUNK = 128
BF = jnp.bfloat16
F32 = jnp.float32
VMEM_LIMIT = 60 * 1024 * 1024


def pick_tile(rows):
    for tile in (256, 128):
        if rows % tile == 0:
            return tile
    return rows


def dot(a, b, dims=((1,), (0,))):
    return lax.dot_general(a, b, (dims, ((), ())), preferred_element_type=F32)


def log1m(k):
    acc = jnp.full_like(k, 1.0 / 9.0)
    for n in range(8, 0, -1):
        acc = acc * k + 1.0 / n
    return -k * acc


def sigmoid(x):
    return 1.0 / (1.0 + jnp.exp(-x))


def front_kernel(
    x_ref, gain_ref, wp_ref, wq_ref, wf_ref, wv_ref, wo_ref, lb_ref, extra_ref,
    pool_ref, rl_ref, qc_ref, og_ref, tot_ref, st_ref,
    run_ref,
):
    step = pl.program_id(0)
    heads, hk = st_ref.shape[0], st_ref.shape[1]

    @pl.when(step == 0)
    def _():
        st_ref[...] = jnp.zeros_like(st_ref)
        run_ref[...] = jnp.zeros_like(run_ref)

    x = x_ref[...].astype(F32)
    scale = lax.rsqrt(jnp.mean(x * x, axis=-1, keepdims=True) + NORM_EPS)
    normed = (x * scale * gain_ref[...]).astype(BF)
    pool_ref[...] = dot(normed, wp_ref[...]).astype(BF)
    og_ref[...] = dot(normed, wo_ref[...]).astype(BF)
    q_raw = dot(normed, wq_ref[...])
    f_raw = dot(normed, wf_ref[...])
    value = dot(normed, wv_ref[...]).astype(BF)
    gap = 1.0 - lb_ref[...]
    q_in = q_raw * sigmoid(q_raw)
    k_in = gap * sigmoid(-f_raw)
    extra = extra_ref[...]
    rows = x.shape[0]
    log_f = log1m(k_in) + jnp.concatenate(
        [jnp.broadcast_to(extra[:, h : h + 1], (rows, hk)) for h in range(heads)], axis=1
    )
    chunk = min(CHUNK, rows)
    t_idx = lax.broadcasted_iota(jnp.int32, (chunk, chunk), 0)
    s_idx = lax.broadcasted_iota(jnp.int32, (chunk, chunk), 1)
    causal = t_idx >= s_idx
    tril = causal.astype(F32).astype(BF)
    for c in range(rows // chunk):
        r = slice(c * chunk, (c + 1) * chunk)
        lf = log_f[r]
        hi = lf.astype(BF)
        lo = (lf - hi.astype(F32)).astype(BF)
        cum = dot(tril, hi) + dot(tril, lo)
        mid = cum[chunk // 2 - 1 : chunk // 2]
        last = cum[chunk - 1 : chunk]
        run = run_ref[...]
        e1 = jnp.exp(cum - mid)
        q_rel = q_in[r] * e1
        k_rel = k_in[r] * jnp.exp(mid - cum)
        q_start = q_rel * jnp.exp(mid)
        k_end = (k_rel * jnp.exp(last - mid)).astype(BF)
        decay = jnp.exp(last)
        qc_ref[r, :] = (q_start * jnp.exp(run)).astype(BF)
        run_ref[...] = run + last
        q_rel = q_rel.astype(BF)
        k_rel = k_rel.astype(BF)
        q_start = q_start.astype(BF)
        for h in range(heads):
            cols = slice(h * hk, (h + 1) * hk)
            vv = value[r, cols]
            scores = dot(q_rel[:, cols], k_rel[:, cols], ((1,), (1,)))
            scores = jnp.where(causal, scores, 0.0).astype(BF)
            st = st_ref[h]
            rl_ref[r, cols] = dot(scores, vv) + dot(q_start[:, cols], st.astype(BF), ((1,), (1,)))
            st_ref[h] = st * decay[:, cols] + dot(vv, k_end[:, cols], ((0,), (0,)))
    tot_ref[...] = run_ref[...]


def back_kernel(
    idx_ref, pool_ref, rl_ref, qc_ref, og_ref, halo_ref, tots_ref, sts_ref, init_ref, rgain_ref,
    mix_ref, pscale_ref,
    y_ref,
    st_ref, prev_ref,
):
    step = pl.program_id(0)
    heads, hk = init_ref.shape[0], init_ref.shape[1]
    me, group = idx_ref[0], idx_ref[1]
    rows, width = pool_ref.shape

    @pl.when(step == 0)
    def _():
        prev_ref[...] = halo_ref[...]
        for h in range(heads):
            st_ref[h] = init_ref[h].T

        @pl.loop(0, me)
        def _(k):
            for h in range(heads):
                decay = jnp.exp(tots_ref[k, :, h * hk : (h + 1) * hk])
                st_ref[h] = st_ref[h] * decay + sts_ref[k, h].astype(F32)

    groups, gw = mix_ref.shape[0], mix_ref.shape[1]
    pool_in = pool_ref[...]
    prev = prev_ref[...]
    t_idx = lax.broadcasted_iota(jnp.int32, (rows, rows), 0)
    s_idx = lax.broadcasted_iota(jnp.int32, (rows, rows), 1)
    tp_idx = lax.broadcasted_iota(jnp.int32, (rows, HALO), 0)
    sp_idx = lax.broadcasted_iota(jnp.int32, (rows, HALO), 1)
    pos = (me * pl.num_programs(0) + step) * rows + lax.broadcasted_iota(jnp.int32, (rows, 1), 0)
    for g in range(groups):
        window = jnp.int32(2) << (group * groups + g)
        cols = slice(g * gw, (g + 1) * gw)
        band = jnp.where((t_idx >= s_idx) & (t_idx - s_idx < window), 1.0, 0.0).astype(BF)
        band_prev = jnp.where(tp_idx + HALO - sp_idx < window, 1.0, 0.0).astype(BF)
        total = dot(band, pool_in[:, cols]) + dot(band_prev, prev[:, cols])
        reach = jnp.minimum(pos + 1, window).astype(F32)
        pooled = (total / reach - pool_in[:, cols].astype(F32)).astype(BF)
        y_ref[:, cols] = (dot(pooled, mix_ref[g]) * pscale_ref[:, cols]).astype(BF)
    prev_ref[...] = pool_in[rows - HALO :]
    out_gate = og_ref[...].astype(F32)
    gate = out_gate * sigmoid(out_gate) * rgain_ref[...]
    for h in range(heads):
        cols = slice(h * hk, (h + 1) * hk)
        rec = rl_ref[:, cols] + dot(qc_ref[:, cols], st_ref[h].astype(BF), ((1,), (1,)))
        rec = rec * lax.rsqrt(jnp.mean(rec * rec, axis=-1, keepdims=True) + NORM_EPS)
        y_ref[:, width + h * hk : width + (h + 1) * hk] = (rec * gate[:, cols]).astype(BF)


def per_device(
    inputs, norm_gain, pool_weight, query_weight, forget_weight, value_weight, outgate_weight,
    pool_mix, pool_scale, lower_bound, extra_decay, recur_gain, init_state, out_pool, out_recur,
):
    rows, d = inputs.shape
    width = pool_weight.shape[1]
    rwidth = query_weight.shape[1]
    heads, hk = init_state.shape[0], init_state.shape[1]
    tile = pick_tile(rows)
    steps = rows // tile
    w_out = lax.all_gather(jnp.concatenate([out_pool, out_recur], axis=0), "tp", axis=0, tiled=True)

    def rowed(w):
        return pl.BlockSpec((tile, w), lambda i: (i, 0))

    def whole(*shape):
        return pl.BlockSpec(shape, lambda i: (0,) * len(shape))

    params = pltpu.CompilerParams(
        dimension_semantics=("arbitrary",), vmem_limit_bytes=VMEM_LIMIT
    )
    pool_in, rl, qc, og, tot, st = pl.pallas_call(
        front_kernel,
        grid=(steps,),
        in_specs=[rowed(d), whole(1, d), whole(d, width)]
        + [whole(d, rwidth)] * 4
        + [whole(1, rwidth), rowed(heads)],
        out_specs=[rowed(width), rowed(rwidth), rowed(rwidth), rowed(rwidth), whole(1, rwidth), whole(heads, hk, hk)],
        out_shape=[
            jax.ShapeDtypeStruct((rows, width), BF),
            jax.ShapeDtypeStruct((rows, rwidth), F32),
            jax.ShapeDtypeStruct((rows, rwidth), BF),
            jax.ShapeDtypeStruct((rows, rwidth), BF),
            jax.ShapeDtypeStruct((1, rwidth), F32),
            jax.ShapeDtypeStruct((heads, hk, hk), F32),
        ],
        scratch_shapes=[pltpu.VMEM((1, rwidth), F32)],
        compiler_params=params,
        cost_estimate=pl.CostEstimate(
            flops=2 * rows * d * (width + 4 * rwidth), bytes_accessed=2 * rows * d, transcendentals=0
        ),
    )(
        inputs, norm_gain[None], pool_weight, query_weight, forget_weight, value_weight,
        outgate_weight, lower_bound[None], extra_decay,
    )
    n = lax.axis_size("sp")
    halo = lax.ppermute(pool_in[rows - HALO :], "sp", [(i, i + 1) for i in range(n - 1)])
    tots = lax.all_gather(tot, "sp")
    sts = lax.all_gather(st.astype(BF), "sp")
    idx = jnp.stack([lax.axis_index("sp"), lax.axis_index("tp")]).astype(jnp.int32)
    y = pl.pallas_call(
        back_kernel,
        grid=(steps,),
        in_specs=[
            pl.BlockSpec(memory_space=pltpu.SMEM),
            rowed(width), rowed(rwidth), rowed(rwidth), rowed(rwidth),
            whole(HALO, width), whole(n, 1, rwidth), whole(n, heads, hk, hk), whole(heads, hk, hk),
            whole(1, rwidth), whole(*pool_mix.shape), whole(1, width),
        ],
        out_specs=rowed(width + rwidth),
        out_shape=jax.ShapeDtypeStruct((rows, width + rwidth), BF),
        scratch_shapes=[pltpu.VMEM((heads, hk, hk), F32), pltpu.VMEM((HALO, width), BF)],
        compiler_params=params,
        cost_estimate=pl.CostEstimate(
            flops=2 * rows * width * width * 2, bytes_accessed=8 * rows * width, transcendentals=0
        ),
    )(idx, pool_in, rl, qc, og, halo, tots, sts, init_state, recur_gain[None], pool_mix, pool_scale[None])
    seen = lax.all_to_all(y, "tp", split_axis=0, concat_axis=1, tiled=True)
    return jnp.dot(seen, w_out, preferred_element_type=F32).astype(BF)


def solution(mesh):
    in_specs = (
        P("sp", None), P(), P(None, "tp"), P(None, "tp"), P(None, "tp"), P(None, "tp"),
        P(None, "tp"), P("tp", None, None), P("tp"), P("tp"), P("sp", "tp"), P("tp"),
        P("tp", None, None), P("tp", None), P("tp", None),
    )
    return jax.shard_map(
        per_device, mesh=mesh, in_specs=in_specs, out_specs=P(("sp", "tp"), None), check_vma=False
    )
```

```python
import functools
import jax
import jax.numpy as jnp
from jax import lax
from jax.experimental import pallas as pl
from jax.experimental.pallas import tpu as pltpu
from jax.sharding import PartitionSpec as P

NORM_EPS = 1e-05
HALO = 16
CHUNK = 128
BF = jnp.bfloat16
F32 = jnp.float32
VMEM_LIMIT = 60 * 1024 * 1024


def dot(a, b, dims=((1,), (0,))):
    return lax.dot_general(a, b, (dims, ((), ())), preferred_element_type=F32)


def log1m(k):
    acc = jnp.full_like(k, 1.0 / 9.0)
    for n in range(8, 0, -1):
        acc = acc * k + 1.0 / n
    return -k * acc


def sigmoid(x):
    return 1.0 / (1.0 + jnp.exp(-x))


MESH = pl.DeviceIdType.MESH
PARTS = 4
SEM_D, SEM_X, SEM_F, SEM_Y, SEM_G, SEM_H, SEM_S, SEM_P, SEM_R = 0, 1, 5, 9, 13, 17, 18, 19, 22
SEMS = 25


def layer_kernel(
    n_sp, n_tp, steps,
    x_ref, gain_ref, wp_ref, wq_ref, wf_ref, wv_ref, wo_ref, lb_ref, extra_ref,
    tail_ref, op_ref, or_ref, init_ref, rgain_ref, mix_ref, pscale_ref,
    out_ref,
    run_ref, st_ref, rl_ref, qc_ref, og_ref, pin_ref, ypool_ref, yrec_ref, pgot_ref, rgot_ref,
    wg_ref, acc_ref, xhalo_ref, sbuf_ref, spair_ref, psend_ref, pgather_ref,
    send_sem, recv_sem, s2_send, s2_recv, loc_sem,
):
    step = pl.program_id(0)
    heads, hk = init_ref.shape[0], init_ref.shape[1]
    tile = x_ref.shape[0]
    gw = op_ref.shape[0]
    half = gw // PARTS
    n_pairs = n_sp // 2
    sp, tp = lax.axis_index("sp"), lax.axis_index("tp")
    hi_t, lo_t = tp // 2, tp % 2
    pair, par = sp // 2, sp % 2
    mate = hi_t * 2 + (1 - lo_t)
    cross = (1 - hi_t) * 2 + lo_t
    diag = (1 - hi_t) * 2 + (1 - lo_t)
    twin = pair * 2 + (1 - par)
    following = lax.rem(sp + 1, n_sp)

    def rdma(src, dst, sem, to):
        return pltpu.make_async_remote_copy(
            src_ref=src, dst_ref=dst, send_sem=send_sem.at[sem], recv_sem=recv_sem.at[sem],
            device_id=to, device_id_type=MESH,
        )

    def w_copy(slot, parity, c, sem, to):
        ref = wg_ref.at[slot, pl.ds(pl.multiple_of(parity * gw + c * half, half), half)]
        return rdma(ref, ref, sem + c, to)

    def copy_d():
        return rdma(wg_ref.at[tp], wg_ref.at[tp], SEM_D, (sp, mate))

    def copy_x(c):
        return w_copy(tp, par, c, SEM_X, (sp, cross))

    def copy_f(c):
        return w_copy(cross, par, c, SEM_F, (sp, mate))

    def copy_y(c):
        return w_copy(cross, par, c, SEM_Y, (twin, tp))

    def copy_g(c):
        return w_copy(cross, 1 - par, c, SEM_G, (sp, mate))

    def copy_h():
        return rdma(tail_ref, xhalo_ref, SEM_H, (following, tp))

    def copy_s():
        return rdma(sbuf_ref, spair_ref, SEM_S, (twin, tp))

    relations = (diag, cross, mate)

    def copy_p(r):
        return rdma(ypool_ref.at[relations[r]], pgot_ref.at[tp], SEM_P + r, (sp, relations[r]))

    def copy_r(r):
        return rdma(yrec_ref.at[relations[r]], rgot_ref.at[tp], SEM_R + r, (sp, relations[r]))

    def copy_2(k):
        to = lax.rem(pair + k, n_pairs)
        return pltpu.make_async_remote_copy(
            src_ref=psend_ref, dst_ref=pgather_ref.at[pair], send_sem=s2_send.at[k],
            recv_sem=s2_recv.at[pair], device_id=(to * 2 + par, tp), device_id_type=MESH,
        )

    def got_2(p):
        return pltpu.make_async_remote_copy(
            src_ref=psend_ref, dst_ref=pgather_ref.at[p], send_sem=s2_send.at[0],
            recv_sem=s2_recv.at[p], device_id=(p * 2 + par, tp), device_id_type=MESH,
        )

    def local_w():
        return (
            pltpu.make_async_copy(op_ref, wg_ref.at[tp, pl.ds(0, gw)], loc_sem.at[0]),
            pltpu.make_async_copy(or_ref, wg_ref.at[tp, pl.ds(gw, gw)], loc_sem.at[1]),
        )

    @pl.when(step == 0)
    def _():
        for copy in local_w():
            copy.start()
        barrier = pltpu.get_barrier_semaphore()
        for k in range(1, n_tp):
            pl.semaphore_signal(barrier, inc=1, device_id=(sp, lax.rem(tp + k, n_tp)), device_id_type=MESH)
        for k in range(1, n_sp):
            pl.semaphore_signal(barrier, inc=1, device_id=(lax.rem(sp + k, n_sp), tp), device_id_type=MESH)
        pl.semaphore_wait(barrier, n_tp - 1 + n_sp - 1)
        copy_h().start()
        for copy in local_w():
            copy.wait()
        for c in range(PARTS):
            copy_x(c).start()
        copy_d().start()
        st_ref[...] = jnp.zeros_like(st_ref)
        run_ref[...] = jnp.zeros_like(run_ref)

    def norm(x):
        x = x.astype(F32)
        scale = lax.rsqrt(jnp.mean(x * x, axis=-1, keepdims=True) + NORM_EPS)
        return (x * scale * gain_ref[...]).astype(BF)

    def pooling(index):
        base = pl.multiple_of(index * tile, HALO)
        rows = pin_ref[pl.ds(base, tile + HALO), :]
        t_idx = lax.broadcasted_iota(jnp.int32, (tile, tile + HALO), 0)
        j_idx = lax.broadcasted_iota(jnp.int32, (tile, tile + HALO), 1)
        back = t_idx + HALO - j_idx
        pos = (sp * steps + index) * tile + lax.broadcasted_iota(jnp.int32, (tile, 1), 0)
        groups, width = mix_ref.shape[0], mix_ref.shape[1]
        for g in range(groups):
            cols = slice(g * width, (g + 1) * width)
            group = tp * groups + g
            window = jnp.int32(2)
            for level in range(1, groups * n_tp):
                window = jnp.where(group >= level, 2 ** (level + 1), window)
            band = jnp.where((back >= 0) & (back < window), 1.0, 0.0).astype(BF)
            total = dot(band, rows[:, cols])
            reach = jnp.minimum(pos + 1, window).astype(F32)
            pooled = (total / reach - rows[HALO:, cols].astype(F32)).astype(BF)
            ypool_ref[index, :, cols] = (dot(pooled, mix_ref[g]) * pscale_ref[:, cols]).astype(BF)

    @pl.when(step == 1)
    def _():
        copy_h().wait_recv()
        halo = dot(norm(xhalo_ref[...]), wp_ref[...])
        pin_ref[0:HALO, :] = jnp.where(sp > 0, halo, 0.0).astype(BF)

    @pl.when(step > 0)
    def _():
        pooling(step - 1)

    normed = norm(x_ref[...])
    base = pl.multiple_of(step * tile, HALO)
    pin_ref[pl.ds(base + HALO, tile), :] = dot(normed, wp_ref[...]).astype(BF)
    og_ref[pl.ds(base, tile), :] = dot(normed, wo_ref[...]).astype(BF)
    q_raw = dot(normed, wq_ref[...])
    f_raw = dot(normed, wf_ref[...])
    value = dot(normed, wv_ref[...]).astype(BF)
    gap = 1.0 - lb_ref[...]
    q_in = q_raw * sigmoid(q_raw)
    k_in = gap * sigmoid(-f_raw)
    extra = extra_ref[...]
    log_f = log1m(k_in) + jnp.concatenate(
        [jnp.broadcast_to(extra[:, h : h + 1], (tile, hk)) for h in range(heads)], axis=1
    )
    chunk = CHUNK
    t_idx = lax.broadcasted_iota(jnp.int32, (chunk, chunk), 0)
    s_idx = lax.broadcasted_iota(jnp.int32, (chunk, chunk), 1)
    causal = t_idx >= s_idx
    tril = causal.astype(F32).astype(BF)
    for c in range(tile // chunk):
        r = slice(c * chunk, (c + 1) * chunk)
        there = pl.ds(pl.multiple_of(base + c * chunk, chunk), chunk)
        lf = log_f[r]
        hi = lf.astype(BF)
        lo = (lf - hi.astype(F32)).astype(BF)
        cum = dot(tril, hi) + dot(tril, lo)
        mid = cum[chunk // 2 - 1 : chunk // 2]
        last = cum[chunk - 1 : chunk]
        run = run_ref[...]
        e1 = jnp.exp(cum - mid)
        q_rel = q_in[r] * e1
        k_rel = k_in[r] * jnp.exp(mid - cum)
        q_start = q_rel * jnp.exp(mid)
        k_end = (k_rel * jnp.exp(last - mid)).astype(BF)
        decay = jnp.exp(last)
        qc_ref[there, :] = (q_start * jnp.exp(run)).astype(BF)
        run_ref[...] = run + last
        q_rel = q_rel.astype(BF)
        k_rel = k_rel.astype(BF)
        q_start = q_start.astype(BF)
        for h in range(heads):
            cols = slice(h * hk, (h + 1) * hk)
            vv = value[r, cols]
            scores = dot(q_rel[:, cols], k_rel[:, cols], ((1,), (1,)))
            scores = jnp.where(causal, scores, 0.0).astype(BF)
            st = st_ref[h]
            rl_ref[there, cols] = dot(scores, vv) + dot(q_start[:, cols], st.astype(BF), ((1,), (1,)))
            st_ref[h] = st * decay[:, cols] + dot(vv, k_end[:, cols], ((0,), (0,)))

    def relay_x(c):
        copy_x(c).wait_recv()
        copy_y(c).start()
        copy_f(c).start()

    for c in range(PARTS - 2):
        @pl.when(step == c + 1)
        def _():
            relay_x(c)

    def write_state(ref, h, decay, state):
        ref[h, 0:hk, :] = state.astype(BF)
        hi = decay.astype(BF).astype(F32)
        rows = jnp.concatenate([hi, decay - hi, jnp.zeros((14, hk), F32)], axis=0)
        ref[h, hk : hk + 16, :] = rows.astype(BF)

    def read_state(value):
        decay = value[hk : hk + 16].astype(F32)
        return decay[0:1] + decay[1:2], value[0:hk].astype(F32)

    @pl.when(step == steps - 1)
    def _():
        for h in range(heads):
            write_state(sbuf_ref, h, jnp.exp(run_ref[:, h * hk : (h + 1) * hk]), st_ref[h])
        copy_s().start()
        relay_x(PARTS - 2)
        pooling(steps - 1)
        for r in range(3):
            copy_p(r).start()
        pgot_ref[tp] = ypool_ref[tp]
        copy_s().wait_recv()
        odd = par == 1
        for h in range(heads):
            own = jnp.exp(run_ref[:, h * hk : (h + 1) * hk]), st_ref[h]
            other = read_state(spair_ref[h])
            early = jnp.where(odd, other[0], own[0]), jnp.where(odd, other[1], own[1])
            late = jnp.where(odd, own[0], other[0]), jnp.where(odd, own[1], other[1])
            write_state(psend_ref, h, early[0] * late[0], early[1] * late[0] + late[1])
        for k in range(1, n_pairs):
            @pl.when(pair + k < n_pairs)
            def _():
                copy_2(k).start()
        relay_x(PARTS - 1)
        for h in range(heads):
            st_ref[h] = init_ref[h].T
        for p in range(n_pairs - 1):
            @pl.when(p < pair)
            def _():
                got_2(p).wait_recv()
                for h in range(heads):
                    decay, state = read_state(pgather_ref[p, h])
                    st_ref[h] = st_ref[h] * decay + state
        for h in range(heads):
            decay, state = read_state(spair_ref[h])
            st_ref[h] = jnp.where(odd, st_ref[h] * decay + state, st_ref[h])

        def finish(index, ref, slot):
            rows = pl.ds(pl.multiple_of(index * tile, HALO), tile)
            out_gate = og_ref[rows, :].astype(F32)
            gate = out_gate * sigmoid(out_gate) * rgain_ref[...]
            for h in range(heads):
                cols = slice(h * hk, (h + 1) * hk)
                rec = rl_ref[rows, cols] + dot(qc_ref[rows, cols], st_ref[h].astype(BF), ((1,), (1,)))
                rec = rec * lax.rsqrt(jnp.mean(rec * rec, axis=-1, keepdims=True) + NORM_EPS)
                ref[slot, :, cols] = (rec * gate[:, cols]).astype(BF)

        for r in range(3):
            finish(relations[r], yrec_ref, relations[r])
            copy_r(r).start()
        finish(tp, rgot_ref, tp)
        for c in range(PARTS):
            copy_y(c).wait_recv()
            copy_g(c).start()
        copy_d().wait_recv()
        for c in range(PARTS):
            copy_f(c).wait_recv()
        for r in range(3):
            copy_p(r).wait_recv()
        for c in range(PARTS):
            copy_g(c).wait_recv()
        rwidth = rgot_ref.shape[2]
        span = min(512, out_ref.shape[1])
        parts_out = out_ref.shape[1] // span

        @pl.loop(0, parts_out)
        def _(j):
            cols = pl.ds(pl.multiple_of(j * span, span), span)
            acc = dot(pgot_ref[0], wg_ref[0, 0:gw, cols])
            for s in range(1, n_tp):
                acc = acc + dot(pgot_ref[s], wg_ref[s, 0:gw, cols])
            acc = acc + dot(rgot_ref[tp], wg_ref[tp, gw : gw + rwidth, cols])
            acc_ref[:, cols] = acc

        for r in range(2, -1, -1):
            copy_r(r).wait_recv()

        @pl.loop(0, parts_out)
        def _(j):
            cols = pl.ds(pl.multiple_of(j * span, span), span)
            acc = acc_ref[:, cols]
            for r in range(3):
                s = relations[r]
                acc = acc + dot(rgot_ref[s], wg_ref[s, gw : gw + rwidth, cols])
            out_ref[:, cols] = acc.astype(BF)

        copy_h().wait_send()
        copy_d().wait_send()
        copy_s().wait_send()
        for c in range(PARTS):
            copy_x(c).wait_send()
            copy_f(c).wait_send()
            copy_y(c).wait_send()
            copy_g(c).wait_send()
        for r in range(3):
            copy_p(r).wait_send()
            copy_r(r).wait_send()
        for k in range(1, n_pairs):
            @pl.when(pair + k < n_pairs)
            def _():
                copy_2(k).wait_send()


def per_device(
    inputs, norm_gain, pool_weight, query_weight, forget_weight, value_weight, outgate_weight,
    pool_mix, pool_scale, lower_bound, extra_decay, recur_gain, init_state, out_pool, out_recur,
):
    rows, d = inputs.shape
    width = pool_weight.shape[1]
    rwidth = query_weight.shape[1]
    heads, hk = init_state.shape[0], init_state.shape[1]
    n_sp, n_tp = lax.axis_size("sp"), lax.axis_size("tp")
    steps = n_tp
    tile = rows // steps
    d_out = out_pool.shape[1]
    n_pairs = n_sp // 2

    def rowed(w):
        return pl.BlockSpec((tile, w), lambda i: (i, 0))

    def whole(*shape):
        return pl.BlockSpec(shape, lambda i: (0,) * len(shape))

    hbm = pl.BlockSpec(memory_space=pl.ANY)
    return pl.pallas_call(
        functools.partial(layer_kernel, n_sp, n_tp, steps),
        grid=(steps,),
        in_specs=[rowed(d), whole(1, d), whole(d, width)]
        + [whole(d, rwidth)] * 4
        + [whole(1, rwidth), rowed(heads), hbm, hbm, hbm, whole(heads, hk, hk), whole(1, rwidth)]
        + [whole(*pool_mix.shape), whole(1, width)],
        out_specs=whole(tile, d_out),
        out_shape=jax.ShapeDtypeStruct((tile, d_out), BF),
        scratch_shapes=[
            pltpu.VMEM((1, rwidth), F32),
            pltpu.VMEM((heads, hk, hk), F32),
            pltpu.VMEM((rows, rwidth), F32),
            pltpu.VMEM((rows, rwidth), BF),
            pltpu.VMEM((rows, rwidth), BF),
            pltpu.VMEM((rows + HALO, width), BF),
            pltpu.VMEM((n_tp, tile, width), BF),
            pltpu.VMEM((n_tp, tile, rwidth), BF),
            pltpu.VMEM((n_tp, tile, width), BF),
            pltpu.VMEM((n_tp, tile, rwidth), BF),
            pltpu.VMEM((n_tp, width + rwidth, d_out), BF),
            pltpu.VMEM((tile, d_out), F32),
            pltpu.VMEM((HALO, d), BF),
            pltpu.VMEM((heads, hk + 16, hk), BF),
            pltpu.VMEM((heads, hk + 16, hk), BF),
            pltpu.VMEM((heads, hk + 16, hk), BF),
            pltpu.VMEM((n_pairs, heads, hk + 16, hk), BF),
            pltpu.SemaphoreType.DMA((SEMS,)),
            pltpu.SemaphoreType.DMA((SEMS,)),
            pltpu.SemaphoreType.DMA((n_pairs,)),
            pltpu.SemaphoreType.DMA((n_pairs,)),
            pltpu.SemaphoreType.DMA((2,)),
        ],
        compiler_params=pltpu.CompilerParams(
            dimension_semantics=("arbitrary",), vmem_limit_bytes=VMEM_LIMIT, collective_id=0,
            has_side_effects=True,
        ),
    )(
        inputs, norm_gain[None], pool_weight, query_weight, forget_weight, value_weight,
        outgate_weight, lower_bound[None], extra_decay, inputs[rows - HALO :], out_pool, out_recur,
        init_state, recur_gain[None], pool_mix, pool_scale[None],
    )


def solution(mesh):
    in_specs = (
        P("sp", None), P(), P(None, "tp"), P(None, "tp"), P(None, "tp"), P(None, "tp"),
        P(None, "tp"), P("tp", None, None), P("tp"), P("tp"), P("sp", "tp"), P("tp"),
        P("tp", None, None), P("tp", None), P("tp", None),
    )
    return jax.shard_map(
        per_device, mesh=mesh, in_specs=in_specs, out_specs=P(("sp", "tp"), None), check_vma=False
    )
```

```python
import functools
import jax
import jax.numpy as jnp
from jax import lax
from jax.experimental import pallas as pl
from jax.experimental.pallas import tpu as pltpu
from jax.sharding import PartitionSpec as P

NORM_EPS = 1e-05
HALO = 16
CHUNK = 128
BF = jnp.bfloat16
F32 = jnp.float32
VMEM_LIMIT = 60 * 1024 * 1024


def dot(a, b, dims=((1,), (0,))):
    return lax.dot_general(a, b, (dims, ((), ())), preferred_element_type=F32)


def log1m(k):
    acc = jnp.full_like(k, 1.0 / 9.0)
    for n in range(8, 0, -1):
        acc = acc * k + 1.0 / n
    return -k * acc


def sigmoid(x):
    return 1.0 / (1.0 + jnp.exp(-x))


MESH = pl.DeviceIdType.MESH
PARTS = 4
SEM_D, SEM_X, SEM_F, SEM_Y, SEM_G, SEM_H, SEM_S, SEM_P, SEM_R = 0, 1, 5, 9, 13, 17, 18, 19, 22
SEMS = 25


def layer_kernel(
    n_sp, n_tp, steps,
    x_ref, gain_ref, wp_ref, wq_ref, wf_ref, wv_ref, wo_ref, lb_ref, extra_ref,
    tail_ref, op_ref, or_ref, init_ref, rgain_ref, mix_ref, pscale_ref,
    out_ref,
    run_ref, st_ref, rl_ref, qc_ref, og_ref, pin_ref, ypool_ref, yrec_ref, pgot_ref, rgot_ref,
    wg_ref, acc_ref, xhalo_ref, sbuf_ref, spair_ref, psend_ref, pgather_ref,
    send_sem, recv_sem, s2_send, s2_recv, loc_sem,
):
    step = pl.program_id(0)
    heads, hk = init_ref.shape[0], init_ref.shape[1]
    tile = x_ref.shape[0]
    gw = op_ref.shape[0]
    half = gw // PARTS
    n_pairs = n_sp // 2
    sp, tp = lax.axis_index("sp"), lax.axis_index("tp")
    hi_t, lo_t = tp // 2, tp % 2
    pair, par = sp // 2, sp % 2
    mate = hi_t * 2 + (1 - lo_t)
    cross = (1 - hi_t) * 2 + lo_t
    diag = (1 - hi_t) * 2 + (1 - lo_t)
    twin = pair * 2 + (1 - par)
    following = lax.rem(sp + 1, n_sp)

    def rdma(src, dst, sem, to):
        return pltpu.make_async_remote_copy(
            src_ref=src, dst_ref=dst, send_sem=send_sem.at[sem], recv_sem=recv_sem.at[sem],
            device_id=to, device_id_type=MESH,
        )

    def w_copy(slot, parity, c, sem, to):
        ref = wg_ref.at[slot, pl.ds(pl.multiple_of(parity * gw + c * half, half), half)]
        return rdma(ref, ref, sem + c, to)

    def copy_d():
        return rdma(wg_ref.at[tp], wg_ref.at[tp], SEM_D, (sp, mate))

    def copy_x(c):
        return w_copy(tp, par, c, SEM_X, (sp, cross))

    def copy_f(c):
        return w_copy(cross, par, c, SEM_F, (sp, mate))

    def copy_y(c):
        return w_copy(cross, par, c, SEM_Y, (twin, tp))

    def copy_g(c):
        return w_copy(cross, 1 - par, c, SEM_G, (sp, mate))

    def copy_h():
        rows = tail_ref.shape[0]
        return rdma(tail_ref.at[pl.ds(rows - HALO, HALO)], xhalo_ref, SEM_H, (following, tp))

    def copy_s():
        return rdma(sbuf_ref, spair_ref, SEM_S, (twin, tp))

    relations = (diag, cross, mate)

    def copy_p(r):
        return rdma(ypool_ref.at[relations[r]], pgot_ref.at[tp], SEM_P + r, (sp, relations[r]))

    def copy_r(r):
        return rdma(yrec_ref.at[relations[r]], rgot_ref.at[tp], SEM_R + r, (sp, relations[r]))

    def copy_2(k):
        to = lax.rem(pair + k, n_pairs)
        return pltpu.make_async_remote_copy(
            src_ref=psend_ref, dst_ref=pgather_ref.at[pair], send_sem=s2_send.at[k],
            recv_sem=s2_recv.at[pair], device_id=(to * 2 + par, tp), device_id_type=MESH,
        )

    def got_2(p):
        return pltpu.make_async_remote_copy(
            src_ref=psend_ref, dst_ref=pgather_ref.at[p], send_sem=s2_send.at[0],
            recv_sem=s2_recv.at[p], device_id=(p * 2 + par, tp), device_id_type=MESH,
        )

    def local_w():
        return (
            pltpu.make_async_copy(op_ref, wg_ref.at[tp, pl.ds(0, gw)], loc_sem.at[0]),
            pltpu.make_async_copy(or_ref, wg_ref.at[tp, pl.ds(gw, gw)], loc_sem.at[1]),
        )

    @pl.when(step == 0)
    def _():
        for copy in local_w():
            copy.start()
        barrier = pltpu.get_barrier_semaphore()
        for k in range(1, n_tp):
            pl.semaphore_signal(barrier, inc=1, device_id=(sp, lax.rem(tp + k, n_tp)), device_id_type=MESH)
        for k in range(1, n_sp):
            pl.semaphore_signal(barrier, inc=1, device_id=(lax.rem(sp + k, n_sp), tp), device_id_type=MESH)
        st_ref[...] = jnp.zeros_like(st_ref)
        run_ref[...] = jnp.zeros_like(run_ref)

    def norm(x):
        x = x.astype(F32)
        scale = lax.rsqrt(jnp.mean(x * x, axis=-1, keepdims=True) + NORM_EPS)
        return (x * scale * gain_ref[...]).astype(BF)

    def pooling(index):
        base = pl.multiple_of(index * tile, HALO)
        rows = pin_ref[pl.ds(base, tile + HALO), :]
        t_idx = lax.broadcasted_iota(jnp.int32, (tile, tile + HALO), 0)
        j_idx = lax.broadcasted_iota(jnp.int32, (tile, tile + HALO), 1)
        back = t_idx + HALO - j_idx
        pos = (sp * steps + index) * tile + lax.broadcasted_iota(jnp.int32, (tile, 1), 0)
        groups, width = mix_ref.shape[0], mix_ref.shape[1]
        for g in range(groups):
            cols = slice(g * width, (g + 1) * width)
            group = tp * groups + g
            window = jnp.int32(2)
            for level in range(1, groups * n_tp):
                window = jnp.where(group >= level, 2 ** (level + 1), window)
            band = jnp.where((back >= 0) & (back < window), 1.0, 0.0).astype(BF)
            total = dot(band, rows[:, cols])
            reach = jnp.minimum(pos + 1, window).astype(F32)
            pooled = (total / reach - rows[HALO:, cols].astype(F32)).astype(BF)
            ypool_ref[index, :, cols] = (dot(pooled, mix_ref[g]) * pscale_ref[:, cols]).astype(BF)

    normed = norm(x_ref[...])
    base = pl.multiple_of(step * tile, HALO)
    pin_ref[pl.ds(base + HALO, tile), :] = dot(normed, wp_ref[...]).astype(BF)
    og_ref[pl.ds(base, tile), :] = dot(normed, wo_ref[...]).astype(BF)
    q_raw = dot(normed, wq_ref[...])
    f_raw = dot(normed, wf_ref[...])
    value = dot(normed, wv_ref[...]).astype(BF)

    @pl.when(step == 0)
    def _():
        pl.semaphore_wait(pltpu.get_barrier_semaphore(), n_tp - 1 + n_sp - 1)
        copy_h().start()
        for copy in local_w():
            copy.wait()
        for c in range(PARTS):
            copy_x(c).start()
        copy_d().start()

    @pl.when(step == 1)
    def _():
        copy_h().wait_recv()
        halo = dot(norm(xhalo_ref[...]), wp_ref[...])
        pin_ref[0:HALO, :] = jnp.where(sp > 0, halo, 0.0).astype(BF)

    @pl.when(step > 0)
    def _():
        pooling(step - 1)

    gap = 1.0 - lb_ref[...]
    q_in = q_raw * sigmoid(q_raw)
    k_in = gap * sigmoid(-f_raw)
    extra = jnp.concatenate([extra_ref[...], jnp.zeros((8 - heads, tile), F32)], axis=0).T
    log_f = log1m(k_in) + jnp.concatenate(
        [jnp.broadcast_to(extra[:, h : h + 1], (tile, hk)) for h in range(heads)], axis=1
    )
    chunk = CHUNK
    t_idx = lax.broadcasted_iota(jnp.int32, (chunk, chunk), 0)
    s_idx = lax.broadcasted_iota(jnp.int32, (chunk, chunk), 1)
    causal = t_idx >= s_idx
    tril = causal.astype(F32).astype(BF)
    for c in range(tile // chunk):
        r = slice(c * chunk, (c + 1) * chunk)
        there = pl.ds(pl.multiple_of(base + c * chunk, chunk), chunk)
        lf = log_f[r]
        hi = lf.astype(BF)
        lo = (lf - hi.astype(F32)).astype(BF)
        cum = dot(tril, hi) + dot(tril, lo)
        mid = cum[chunk // 2 - 1 : chunk // 2]
        last = cum[chunk - 1 : chunk]
        run = run_ref[...]
        e1 = jnp.exp(cum - mid)
        q_rel = q_in[r] * e1
        k_rel = k_in[r] * jnp.exp(mid - cum)
        q_start = q_rel * jnp.exp(mid)
        k_end = (k_rel * jnp.exp(last - mid)).astype(BF)
        decay = jnp.exp(last)
        qc_ref[there, :] = (q_start * jnp.exp(run)).astype(BF)
        run_ref[...] = run + last
        q_rel = q_rel.astype(BF)
        k_rel = k_rel.astype(BF)
        q_start = q_start.astype(BF)
        for h in range(heads):
            cols = slice(h * hk, (h + 1) * hk)
            vv = value[r, cols]
            scores = dot(q_rel[:, cols], k_rel[:, cols], ((1,), (1,)))
            scores = jnp.where(causal, scores, 0.0).astype(BF)
            st = st_ref[h]
            rl_ref[there, cols] = dot(scores, vv) + dot(q_start[:, cols], st.astype(BF), ((1,), (1,)))
            st_ref[h] = st * decay[:, cols] + dot(vv, k_end[:, cols], ((0,), (0,)))

    def relay_x(c):
        copy_x(c).wait_recv()
        copy_y(c).start()
        copy_f(c).start()

    for c in range(PARTS - 2):
        @pl.when(step == c + 1)
        def _():
            relay_x(c)

    def write_state(ref, h, decay, state):
        ref[h, 0:hk, :] = state.astype(BF)
        hi = decay.astype(BF).astype(F32)
        rows = jnp.concatenate([hi, decay - hi, jnp.zeros((14, hk), F32)], axis=0)
        ref[h, hk : hk + 16, :] = rows.astype(BF)

    def read_state(value):
        decay = value[hk : hk + 16].astype(F32)
        return decay[0:1] + decay[1:2], value[0:hk].astype(F32)

    @pl.when(step == steps - 1)
    def _():
        for h in range(heads):
            write_state(sbuf_ref, h, jnp.exp(run_ref[:, h * hk : (h + 1) * hk]), st_ref[h])
        copy_s().start()
        relay_x(PARTS - 2)
        pooling(steps - 1)
        for r in range(3):
            copy_p(r).start()
        pgot_ref[tp] = ypool_ref[tp]
        copy_s().wait_recv()
        odd = par == 1
        for h in range(heads):
            own = jnp.exp(run_ref[:, h * hk : (h + 1) * hk]), st_ref[h]
            other = read_state(spair_ref[h])
            early = jnp.where(odd, other[0], own[0]), jnp.where(odd, other[1], own[1])
            late = jnp.where(odd, own[0], other[0]), jnp.where(odd, own[1], other[1])
            write_state(psend_ref, h, early[0] * late[0], early[1] * late[0] + late[1])
        for k in range(1, n_pairs):
            @pl.when(pair + k < n_pairs)
            def _():
                copy_2(k).start()
        relay_x(PARTS - 1)
        for h in range(heads):
            st_ref[h] = init_ref[h].T
        for p in range(n_pairs - 1):
            @pl.when(p < pair)
            def _():
                got_2(p).wait_recv()
                for h in range(heads):
                    decay, state = read_state(pgather_ref[p, h])
                    st_ref[h] = st_ref[h] * decay + state
        for h in range(heads):
            decay, state = read_state(spair_ref[h])
            st_ref[h] = jnp.where(odd, st_ref[h] * decay + state, st_ref[h])

        def finish(index, ref, slot):
            rows = pl.ds(pl.multiple_of(index * tile, HALO), tile)
            out_gate = og_ref[rows, :].astype(F32)
            gate = out_gate * sigmoid(out_gate) * rgain_ref[...]
            for h in range(heads):
                cols = slice(h * hk, (h + 1) * hk)
                rec = rl_ref[rows, cols] + dot(qc_ref[rows, cols], st_ref[h].astype(BF), ((1,), (1,)))
                rec = rec * lax.rsqrt(jnp.mean(rec * rec, axis=-1, keepdims=True) + NORM_EPS)
                ref[slot, :, cols] = (rec * gate[:, cols]).astype(BF)

        for r in range(3):
            finish(relations[r], yrec_ref, relations[r])
            copy_r(r).start()
        finish(tp, rgot_ref, tp)
        for c in range(PARTS):
            copy_y(c).wait_recv()
            copy_g(c).start()
        copy_d().wait_recv()
        for c in range(PARTS):
            copy_f(c).wait_recv()
        for r in range(3):
            copy_p(r).wait_recv()
        copy_r(2).wait_recv()
        for c in range(PARTS):
            copy_g(c).wait_recv()
        rwidth = rgot_ref.shape[2]
        span = min(512, out_ref.shape[1])
        parts_out = out_ref.shape[1] // span

        @pl.loop(0, parts_out)
        def _(j):
            cols = pl.ds(pl.multiple_of(j * span, span), span)
            acc = dot(pgot_ref[0], wg_ref[0, 0:gw, cols])
            for s in range(1, n_tp):
                acc = acc + dot(pgot_ref[s], wg_ref[s, 0:gw, cols])
            for s in (tp, mate):
                acc = acc + dot(rgot_ref[s], wg_ref[s, gw : gw + rwidth, cols])
            acc_ref[:, cols] = acc

        for r in range(2):
            copy_r(r).wait_recv()

        @pl.loop(0, parts_out)
        def _(j):
            cols = pl.ds(pl.multiple_of(j * span, span), span)
            acc = acc_ref[:, cols]
            for r in range(2):
                s = relations[r]
                acc = acc + dot(rgot_ref[s], wg_ref[s, gw : gw + rwidth, cols])
            out_ref[:, cols] = acc.astype(BF)

        copy_h().wait_send()
        copy_d().wait_send()
        copy_s().wait_send()
        for c in range(PARTS):
            copy_x(c).wait_send()
            copy_f(c).wait_send()
            copy_y(c).wait_send()
            copy_g(c).wait_send()
        for r in range(3):
            copy_p(r).wait_send()
            copy_r(r).wait_send()
        for k in range(1, n_pairs):
            @pl.when(pair + k < n_pairs)
            def _():
                copy_2(k).wait_send()


def per_device(
    inputs, norm_gain, pool_weight, query_weight, forget_weight, value_weight, outgate_weight,
    pool_mix, pool_scale, lower_bound, extra_decay, recur_gain, init_state, out_pool, out_recur,
):
    rows, d = inputs.shape
    width = pool_weight.shape[1]
    rwidth = query_weight.shape[1]
    heads, hk = init_state.shape[0], init_state.shape[1]
    n_sp, n_tp = lax.axis_size("sp"), lax.axis_size("tp")
    steps = n_tp
    tile = rows // steps
    d_out = out_pool.shape[1]
    n_pairs = n_sp // 2

    def rowed(w):
        return pl.BlockSpec((tile, w), lambda i: (i, 0))

    def whole(*shape):
        return pl.BlockSpec(shape, lambda i: (0,) * len(shape))

    hbm = pl.BlockSpec(memory_space=pl.ANY)
    return pl.pallas_call(
        functools.partial(layer_kernel, n_sp, n_tp, steps),
        grid=(steps,),
        in_specs=[rowed(d), whole(1, d), whole(d, width)]
        + [whole(d, rwidth)] * 4
        + [whole(1, rwidth), pl.BlockSpec((heads, tile), lambda i: (0, i)), hbm, hbm, hbm, whole(heads, hk, hk), whole(1, rwidth)]
        + [whole(*pool_mix.shape), whole(1, width)],
        out_specs=whole(tile, d_out),
        out_shape=jax.ShapeDtypeStruct((tile, d_out), BF),
        scratch_shapes=[
            pltpu.VMEM((1, rwidth), F32),
            pltpu.VMEM((heads, hk, hk), F32),
            pltpu.VMEM((rows, rwidth), F32),
            pltpu.VMEM((rows, rwidth), BF),
            pltpu.VMEM((rows, rwidth), BF),
            pltpu.VMEM((rows + HALO, width), BF),
            pltpu.VMEM((n_tp, tile, width), BF),
            pltpu.VMEM((n_tp, tile, rwidth), BF),
            pltpu.VMEM((n_tp, tile, width), BF),
            pltpu.VMEM((n_tp, tile, rwidth), BF),
            pltpu.VMEM((n_tp, width + rwidth, d_out), BF),
            pltpu.VMEM((tile, d_out), F32),
            pltpu.VMEM((HALO, d), BF),
            pltpu.VMEM((heads, hk + 16, hk), BF),
            pltpu.VMEM((heads, hk + 16, hk), BF),
            pltpu.VMEM((heads, hk + 16, hk), BF),
            pltpu.VMEM((n_pairs, heads, hk + 16, hk), BF),
            pltpu.SemaphoreType.DMA((SEMS,)),
            pltpu.SemaphoreType.DMA((SEMS,)),
            pltpu.SemaphoreType.DMA((n_pairs,)),
            pltpu.SemaphoreType.DMA((n_pairs,)),
            pltpu.SemaphoreType.DMA((2,)),
        ],
        compiler_params=pltpu.CompilerParams(
            dimension_semantics=("arbitrary",), vmem_limit_bytes=VMEM_LIMIT, collective_id=0,
            has_side_effects=True,
        ),
    )(
        inputs, norm_gain[None], pool_weight, query_weight, forget_weight, value_weight,
        outgate_weight, lower_bound[None], extra_decay.T, inputs, out_pool, out_recur,
        init_state, recur_gain[None], pool_mix, pool_scale[None],
    )


def solution(mesh):
    in_specs = (
        P("sp", None), P(), P(None, "tp"), P(None, "tp"), P(None, "tp"), P(None, "tp"),
        P(None, "tp"), P("tp", None, None), P("tp"), P("tp"), P("sp", "tp"), P("tp"),
        P("tp", None, None), P("tp", None), P("tp", None),
    )
    return jax.shard_map(
        per_device, mesh=mesh, in_specs=in_specs, out_specs=P(("sp", "tp"), None), check_vma=False
    )
```
